32 devices in a mesh: ep: 4 (over z), tp: 8 (over y, x, core).
Axes of the slice: x: 2, y: 2, z: 4, core: 2. Of those that a mesh axis runs over, the one named last changes fastest.
Arguments:
- tokens: bfloat16 [4096, 2048], P(('ep', 'tp')), may hold values from -40 to 40
- norm_gain: float32 [2048], replicated, may hold values from 0.1 to 1.9
- routes: int32 [4096, 2], P(('ep', 'tp')), may hold values from 0 to 7, all different within a row; in each aligned block of 128 rows (0 to 127, 128 to 255, ...) at most 64 rows name the same one
- gates: float32 [4096, 2], P(('ep', 'tp')), may hold values from 0.25 to 2
- expert_gate: bfloat16 [8, 2048, 512], P('tp'), may hold values from -0.125 to 0.125
- expert_up: bfloat16 [8, 2048, 512], P('tp'), may hold values from -0.125 to 0.125
- expert_down: bfloat16 [8, 512, 2048], P('tp'), may hold values from -0.25 to 0.25
- shared_gate: bfloat16 [2048, 256], replicated, may hold values from -0.125 to 0.125
- shared_up: bfloat16 [2048, 256], replicated, may hold values from -0.125 to 0.125
- shared_down: bfloat16 [256, 2048], replicated, may hold values from -0.375 to 0.375
Outputs:
- mixed: bfloat16 [4096, 2048], P(('ep', 'tp'))
- load: float32 [8], replicated
The draws below stay inside these ranges and needn't reach their ends.
Inputs may be any that keep to these rules, and one draw needn't show every extreme that they name: `routes`: each row names 2 different experts. Among the rows of one device no expert is named by more than 64 rows, and in every draw some expert is named by exactly 64 rows of some device.
All inputs are finite; a program needn't handle non-finite values.
Results may differ from the reference program's by a relative error of at most 0.002.
The reference program's roundings to bfloat16 on the way count: a program that leaves them out, or rounds other values in their place, can miss the bound.
Values may be sent and summed in bfloat16 or wider, within the bound.
No kernel may reach another device: no remote copies, remote signals or barrier semaphores. Data moves between devices by JAX's collectives and lax.ppermute only.
A program may use at most 64 MiB of HBM per device.

```python
import math
import jax
import jax.numpy as jnp
import numpy as np
from jax import lax

D = 2048
EXPERT_UNITS = 512
SHARED = 256
TOPK = 2
TOK_DEV = 128
EXPERTS = 8
CAP = 64
TOKENS = 4096


def draw_tokens(key, part):
    key_values, key_column, key_row = jax.random.split(key, 3)
    column_scale = jnp.exp(jax.random.uniform(key_column, (D,), jnp.float32, jnp.log(0.5), jnp.log(5.0)))
    row_scale = jnp.exp(jax.random.uniform(key_row, (TOKENS, 1), jnp.float32, jnp.log(0.5), jnp.log(2.0)))
    base_values = jnp.clip(jax.random.normal(key_values, (TOKENS, D), jnp.float32), -4.0, 4.0)
    return (base_values * column_scale * row_scale).astype(jnp.bfloat16)


def level_of(stream_key, shape, pieces, low, high):
    level, own = 1.0, jax.random.fold_in(stream_key, 6)
    for axis_at, parts in pieces:
        heights = jnp.exp(jax.random.uniform(jax.random.fold_in(own, axis_at), (parts,), jnp.float32, low / len(pieces), high / len(pieces)))
        level = level * jnp.repeat(heights, shape[axis_at] // parts).reshape([-1 if axis == axis_at else 1 for axis in range(len(shape))])
    return level


def routed_block(own_key, own, number, rows, number_of, top, bound, skew):
    ranking = jax.random.permutation(own_key, number_of)
    crowded, ordinary = load_shares(number_of, rows * top, bound, skew, True), load_shares(number_of, rows * top, bound, skew, False)
    places = jnp.arange(number_of)

    def named(lengths, rotation):
        used = int((lengths > 0).sum())
        fixed = max(1, used // 4)
        passed = fixed + (places - fixed + rotation * (used - fixed)) % max(1, number_of - fixed)
        return jnp.zeros((number_of,), jnp.int32).at[ranking[jnp.where(places < fixed, places, passed)]].set(jnp.asarray(lengths, jnp.int32))

    lengths = jnp.where(number % 4 == 0, named(crowded, number // 4), named(ordinary, number - number // 4 - 1))
    mixed = jax.random.permutation(jax.random.fold_in(own, 3), number_of)
    donor, sink = mixed[0:number_of // 2 * 2:2], mixed[1:number_of // 2 * 2:2]
    slack = jnp.minimum(lengths[donor] - 1, bound - lengths[sink]) // 2
    slack = jnp.where((donor == ranking[0]) | (sink == ranking[0]) | (lengths[sink] == 0), 0, jnp.maximum(slack, 0))
    passed = jax.random.randint(jax.random.fold_in(own, 4), (number_of // 2,), 0, 1 << 20) % (slack + 1)
    lengths = lengths.at[donor].add(-passed).at[sink].add(passed)
    items = jnp.searchsorted(jnp.cumsum(lengths), jnp.arange(rows * top), side="right").astype(jnp.int32)
    table = items.reshape(top, rows).T
    table = table[jax.random.permutation(jax.random.fold_in(own, 1), rows)]
    rotation = jax.random.randint(jax.random.fold_in(own, 2), (rows, 1), 0, top)
    return jnp.take_along_axis(table, (jnp.arange(top)[None, :] + rotation) % top, axis=1)


def load_shares(amount, total, reach, lean, full):
    portions = [(1 << 20) // math.isqrt(grade ** lean) + 1 for grade in range(1, amount + 1)]
    largest = reach if full else min(reach, max(-(-total // amount), total * portions[0] // sum(portions)))
    least = 1 if total - largest >= amount - 1 else 0
    given, rest = [largest] + [least] * (amount - 1), total - largest - least * (amount - 1)
    while rest > 0:
        candidates = [i for i in range(1, amount) if given[i] < largest] or [i for i in range(1, amount) if given[i] < reach]
        whole, budget = sum([portions[i] for i in candidates]), rest
        for i in candidates:
            more = min(reach - given[i], max(1, budget * portions[i] // whole), rest)
            given[i] = given[i] + more
            rest = rest - more
    return np.array(given)


def scatter_about(key, extent, deviation, reach, cuts=(), kind=jnp.bfloat16):
    gain = level_of(key, extent, cuts, -0.22, 0.18) if cuts else 1.0
    drawn = jax.random.normal(key, extent, jnp.float32) * deviation * gain
    return jnp.minimum(jnp.maximum(drawn, -reach), reach).astype(kind)


def setup_inputs(seed: int = 0) -> dict:
    streams_of = jax.random.split(jax.random.key(seed), 11)
    tokens = draw_tokens(jax.random.fold_in(streams_of[10], 71), 0)
    norm_gain = jnp.clip(1.0 + 0.18 * jax.random.normal(streams_of[1], (D,), jnp.float32), 0.1, 1.9)
    routes_keys = jax.random.split(jax.random.fold_in(streams_of[2], 1), TOKENS // TOK_DEV)
    routes_turns = jax.random.permutation(jax.random.fold_in(streams_of[2], 3), TOKENS // TOK_DEV)
    routes = jax.vmap(lambda own, number: routed_block(jax.random.fold_in(streams_of[2], 2), own, number, TOK_DEV, EXPERTS, TOPK, CAP, 2))(routes_keys, routes_turns).reshape((TOKENS, TOPK))
    gates = jnp.clip(0.25 + 1.75 * jax.random.uniform(streams_of[3], (TOKENS, TOPK), jnp.float32) ** level_of(streams_of[3], (TOKENS, TOPK), ((0, 32),), -0.2, 0.2), 0.25, 2.0)
    expert_gate = scatter_about(streams_of[4], (EXPERTS, D, EXPERT_UNITS), D ** -0.5, 0.125, ((0, 8),))
    expert_up = scatter_about(streams_of[5], (EXPERTS, D, EXPERT_UNITS), D ** -0.5, 0.125, ((0, 8),))
    expert_down = scatter_about(streams_of[6], (EXPERTS, EXPERT_UNITS, D), EXPERT_UNITS ** -0.5, 0.25, ((0, 8),))
    shared_gate = scatter_about(streams_of[7], (D, SHARED), D ** -0.5, 0.125)
    shared_up = scatter_about(streams_of[8], (D, SHARED), D ** -0.5, 0.125)
    shared_down = scatter_about(streams_of[9], (SHARED, D), SHARED ** -0.5, 0.375)
    return dict(tokens=tokens, norm_gain=norm_gain, routes=routes, gates=gates, expert_gate=expert_gate, expert_up=expert_up, expert_down=expert_down, shared_gate=shared_gate, shared_up=shared_up, shared_down=shared_down)


block_rows = 512

def layer_normed(token_block, norm_gain):
    values = token_block.astype(jnp.float32)
    center = lax.optimization_barrier(jnp.mean(values, axis=-1, keepdims=True))
    spread = lax.optimization_barrier(jnp.mean(jnp.square(values - center), axis=-1, keepdims=True))
    return ((values - center) * lax.rsqrt(spread + 1e-05) * norm_gain).astype(jnp.bfloat16)

def gated_mlp(row_block, w_gate, w_up, w_down):
    gate_part = jnp.dot(row_block, w_gate, preferred_element_type=jnp.float32)
    up_part = jnp.dot(row_block, w_up, preferred_element_type=jnp.float32)
    hidden = (jax.nn.silu(gate_part) * up_part).astype(jnp.bfloat16)
    return jnp.dot(hidden, w_down, preferred_element_type=jnp.float32)

def reference(tokens, norm_gain, routes, gates, expert_gate, expert_up, expert_down, shared_gate, shared_up, shared_down):
    normed = layer_normed(tokens, norm_gain)
    count_rows, feature_count = normed.shape
    copy_count = count_rows * TOPK
    flat_expert = routes.reshape(-1).astype(jnp.int32)
    flat_token = jnp.repeat(jnp.arange(count_rows, dtype=jnp.int32), TOPK)
    sort_order = jnp.argsort(flat_expert, stable=True).astype(jnp.int32)
    sorted_expert = flat_expert[sort_order]
    counts = lax.optimization_barrier(jnp.sum((flat_expert[:, None] == jnp.arange(EXPERTS, dtype=jnp.int32)[None, :]).astype(jnp.int32), axis=0))
    padded = (counts + block_rows - 1) // block_rows * block_rows
    starts = jnp.cumsum(counts) - counts
    block_ends = jnp.cumsum(padded)
    padded_starts = block_ends - padded
    destination = (padded_starts[sorted_expert] + jnp.arange(copy_count, dtype=jnp.int32) - starts[sorted_expert]).astype(jnp.int32)
    block_count = -(-copy_count // block_rows) + EXPERTS
    slot_token = jnp.full((block_count * block_rows,), count_rows, jnp.int32).at[destination].set(flat_token[sort_order])
    block_expert = jnp.clip(jnp.searchsorted(block_ends, jnp.arange(block_count, dtype=jnp.int32) * block_rows, side='right'), 0, EXPERTS - 1).astype(jnp.int32)
    padded_rows = jnp.concatenate([normed, jnp.zeros((1, feature_count), normed.dtype)], axis=0)

    def run_block(block_item):
        slot_tokens, expert = block_item
        row_block = padded_rows[slot_tokens]
        return gated_mlp(row_block, expert_gate[expert], expert_up[expert], expert_down[expert]).astype(jnp.bfloat16)
    slot_out = lax.map(run_block, (slot_token.reshape(block_count, block_rows), block_expert))
    slot_out = slot_out.reshape(block_count * block_rows, feature_count)
    copy_slot = jnp.zeros((copy_count,), jnp.int32).at[sort_order].set(destination).reshape(count_rows, TOPK)
    routed = jnp.zeros((count_rows, feature_count), jnp.float32)
    for choice_index in range(TOPK):
        picked = slot_out[copy_slot[:, choice_index]].astype(jnp.float32)
        routed = routed + gates[:, choice_index][:, None] * picked
    shared_out = gated_mlp(normed, shared_gate, shared_up, shared_down)
    mixed = (routed + shared_out).astype(jnp.bfloat16)
    load = counts.astype(jnp.float32) * (EXPERTS / (count_rows * TOPK))
    return (mixed, load)
```

```python
import functools

import jax
import jax.numpy as jnp
import numpy as np
from jax import lax
from jax.experimental import pallas as pl
from jax.experimental.pallas import tpu as pltpu
from jax.sharding import PartitionSpec as P

LANES = 128
HBM = pl.BlockSpec(memory_space=pl.ANY)
VMEM = pl.BlockSpec(memory_space=pltpu.VMEM)
SMEM = pl.BlockSpec(memory_space=pltpu.SMEM)
F32 = jnp.float32
BF16 = jnp.bfloat16


def dot(a, b, contract=((1,), (0,))):
    return lax.dot_general(a, b, (contract, ((), ())), preferred_element_type=F32)


def layer_normed(values, gain):
    center = jnp.mean(values, axis=-1, keepdims=True)
    moved = values - center
    spread = jnp.mean(moved * moved, axis=-1, keepdims=True)
    return (moved * lax.rsqrt(spread + 1e-05) * gain).astype(BF16)


def silu(v):
    return v / (1.0 + jnp.exp(-v))


def places(meta, expert, slots):
    rows = meta.shape[0]
    named = ((meta[:, 0:1] == expert) | (meta[:, 1:2] == expert)).astype(F32)
    row = lax.broadcasted_iota(jnp.int32, (rows, rows), 0)
    col = lax.broadcasted_iota(jnp.int32, (rows, rows), 1)
    before = (col < row).astype(F32).astype(BF16)
    rank = dot(before, jnp.broadcast_to(named, (rows, LANES)).astype(BF16))[:, :slots]
    slot = lax.broadcasted_iota(jnp.int32, (rows, slots), 1).astype(F32)
    return jnp.where(rank == slot, named, 0.0).astype(BF16)


def expert_kernel(count, slots, me_ref, gain_ref, *refs):
    blocks = refs[:count]
    wg_hbm, wu_hbm, wd_hbm = refs[count : count + 3]
    outs = refs[count + 3 : 2 * count + 3]
    tally_ref = refs[2 * count + 3]
    normed, wg, wu, wd, sems = refs[2 * count + 4 :]
    width = gain_ref.shape[1]
    loads = [
        pltpu.make_async_copy(src.at[0], dst, sems.at[i])
        for i, (src, dst) in enumerate(((wg_hbm, wg), (wu_hbm, wu), (wd_hbm, wd)))
    ]
    for load in loads:
        load.start()
    expert = me_ref[0].astype(F32)
    tally = jnp.zeros(tally_ref.shape, F32)
    for i, block in enumerate(blocks):
        meta = block[:, width:].astype(F32)
        tally = tally + meta[0:8]
        chosen = dot(places(meta, expert, slots), block[:, :width], ((0,), (0,)))
        normed[i * slots : (i + 1) * slots, :] = layer_normed(chosen, gain_ref[...])
    tally_ref[...] = tally
    loads[0].wait()
    gate = dot(normed[...], wg[...])
    loads[1].wait()
    up = dot(normed[...], wu[...])
    hidden = (silu(gate) * up).astype(BF16)
    loads[2].wait()
    result = dot(hidden, wd[...]).astype(BF16)
    for i, out in enumerate(outs):
        out[...] = result[i * slots : (i + 1) * slots]


def expert_call(me, gain, blocks, slots, wg, wu, wd):
    count = len(blocks)
    width, units = wg.shape[1:]
    return pl.pallas_call(
        functools.partial(expert_kernel, count, slots),
        out_shape=[jax.ShapeDtypeStruct((slots, width), BF16)] * count
        + [jax.ShapeDtypeStruct((8, LANES), F32)],
        in_specs=[SMEM, VMEM] + [VMEM] * count + [HBM] * 3,
        out_specs=[VMEM] * (count + 1),
        scratch_shapes=[
            pltpu.VMEM((count * slots, width), BF16),
            pltpu.VMEM((width, units), BF16),
            pltpu.VMEM((width, units), BF16),
            pltpu.VMEM((units, width), BF16),
            pltpu.SemaphoreType.DMA((3,)),
        ],
        compiler_params=pltpu.CompilerParams(vmem_limit_bytes=40 * 2**20),
        cost_estimate=pl.CostEstimate(
            flops=6 * count * slots * width * units, bytes_accessed=6 * width * units, transcendentals=0
        ),
        name="expert_rows",
    )(me, gain, *blocks, wg, wu, wd)


def shared_kernel(tokens_ref, gain_ref, wg_ref, wu_ref, wd_ref, out_ref):
    normed = layer_normed(tokens_ref[...].astype(F32), gain_ref[...])
    hidden = (silu(dot(normed, wg_ref[...])) * dot(normed, wu_ref[...])).astype(BF16)
    out_ref[...] = dot(hidden, wd_ref[...])


def combine_kernel(count, experts_ref, meta_ref, gates_ref, base_ref, *refs):
    blocks, out_ref = refs[:count], refs[count]
    meta = meta_ref[...].astype(F32)
    total = base_ref[...]
    for i, block in enumerate(blocks):
        expert = experts_ref[i].astype(F32)
        gate = jnp.where(meta[:, 0:1] == expert, gates_ref[:, 0:1], gates_ref[:, 1:2])
        total = total + gate * dot(places(meta, expert, block.shape[0]), block[...])
    out_ref[...] = total.astype(out_ref.dtype)


def combine_call(experts, meta, gates, base, blocks, kind):
    return pl.pallas_call(
        functools.partial(combine_kernel, len(blocks)),
        out_shape=jax.ShapeDtypeStruct(base.shape, kind),
        in_specs=[SMEM] + [VMEM] * (3 + len(blocks)),
        out_specs=VMEM,
        compiler_params=pltpu.CompilerParams(vmem_limit_bytes=24 * 2**20),
        name="combine_rows",
    )(experts, meta, gates, base, *blocks)


def per_device(
    tokens,
    norm_gain,
    routes,
    gates,
    expert_gate,
    expert_up,
    expert_down,
    shared_gate,
    shared_up,
    shared_down,
):
    rows, width = tokens.shape
    top = routes.shape[1]
    groups, planes = lax.axis_size("tp"), lax.axis_size("ep")
    slots = 2 * rows * top // groups
    me = lax.axis_index("tp")
    ids = np.arange(groups)

    def send(value, perm):
        return lax.ppermute(value, "tp", [(int(i), int(perm[i])) for i in ids])

    onehot = (routes.reshape(-1)[:, None] == jnp.arange(groups)[None, :]).astype(F32)
    counts = jnp.sum(onehot, axis=0)
    meta = jnp.concatenate(
        [routes.astype(F32), jnp.broadcast_to(counts[None, :], (rows, groups))], axis=1
    )
    meta = jnp.pad(meta, ((0, 0), (0, LANES - meta.shape[1]))).astype(BF16)
    packed = jnp.concatenate([tokens, meta], axis=1)
    gain = norm_gain.reshape(1, width)

    masks = [1 << b for b in range(1, groups.bit_length() - 1)]
    stages = [[(packed, ids)]]
    known = [(packed, ids)]
    for step in range(len(masks)):
        hop = np.where(ids % 2 == 0, ids ^ masks[step], ids ^ masks[-1 - step])
        fresh = [(send(block, hop), origin[hop]) for block, origin in known]
        known = known + fresh
        if step == 0:
            stages.append(fresh)
        else:
            stages[-1].append(fresh[0])
            stages.append(fresh[1:])
    partner = ids ^ 1
    stages = [
        stage + [(send(block, partner), origin[partner]) for block, origin in stage]
        for stage in stages
    ]

    base = pl.pallas_call(
        shared_kernel,
        out_shape=jax.ShapeDtypeStruct((rows, width), F32),
        in_specs=[VMEM] * 5,
        out_specs=VMEM,
        compiler_params=pltpu.CompilerParams(vmem_limit_bytes=24 * 2**20),
        name="shared_rows",
    )(tokens, gain, shared_gate, shared_up, shared_down)

    mine = me.reshape(1).astype(jnp.int32)
    tally = jnp.zeros((8, LANES), F32)
    returned = []
    for stage in stages:
        *results, part = expert_call(
            mine, gain, [b for b, _ in stage], slots, expert_gate, expert_up, expert_down
        )
        tally = tally + part
        back = []
        for (_, origin), result in zip(stage, results):
            if np.array_equal(origin, ids):
                back.append((result, ids))
            else:
                back.append((send(result, origin), np.argsort(origin)))
        returned.append(back)

    early = [item for back in returned[:-1] for item in back]
    for blocks, kind in ((early, F32), (returned[-1], BF16)):
        experts = jnp.stack([jnp.asarray(origin, jnp.int32)[me] for _, origin in blocks])
        base = combine_call(experts, meta, gates, base, [b for b, _ in blocks], kind)

    total = tally[0:1]
    if planes & (planes - 1):
        total = lax.psum(total, "ep")
    else:
        for bit in range(planes.bit_length() - 1):
            total = total + lax.ppermute(total, "ep", [(i, i ^ (1 << bit)) for i in range(planes)])
    load = total[0, top : top + groups] * (groups / (rows * top * planes * groups))
    return base, load


def solution(mesh):
    placed = (
        P(("ep", "tp"), None),
        P(),
        P(("ep", "tp"), None),
        P(("ep", "tp"), None),
        P("tp", None, None),
        P("tp", None, None),
        P("tp", None, None),
        P(),
        P(),
        P(),
    )
    return jax.shard_map(
        per_device,
        mesh=mesh,
        in_specs=placed,
        out_specs=(P(("ep", "tp"), None), P()),
        check_vma=False,
    )
```

```python
import functools

import jax
import jax.numpy as jnp
import numpy as np
from jax import lax
from jax.experimental import pallas as pl
from jax.experimental.pallas import tpu as pltpu
from jax.sharding import PartitionSpec as P

LANES = 128
VMEM = pl.BlockSpec(memory_space=pltpu.VMEM)
F32 = jnp.float32
BF16 = jnp.bfloat16


def dot(a, b, contract=((1,), (0,))):
    return lax.dot_general(a, b, (contract, ((), ())), preferred_element_type=F32)


def layer_normed(values, gain):
    center = jnp.mean(values, axis=-1, keepdims=True)
    moved = values - center
    spread = jnp.mean(moved * moved, axis=-1, keepdims=True)
    return (moved * lax.rsqrt(spread + 1e-05) * gain).astype(BF16)


def silu(v):
    return v / (1.0 + jnp.exp(-v))


def before_mask(rows):
    row = lax.broadcasted_iota(jnp.int32, (rows, rows), 0)
    col = lax.broadcasted_iota(jnp.int32, (rows, rows), 1)
    return jnp.where(row < col, 1.0, 0.0).astype(BF16)


def places(first, second, expert, slots, before):
    rows = first.shape[1]
    named = jnp.where((first == expert) | (second == expert), 1.0, 0.0)
    rank = dot(jnp.broadcast_to(named, (8, rows)).astype(BF16), before)[0:1]
    slot = lax.broadcasted_iota(jnp.int32, (slots, rows), 0).astype(F32)
    return jnp.where((rank == slot) & (named > 0.0), 1.0, 0.0)


def origin_id(masks):
    me = lax.axis_index("tp")
    return jnp.where(me % 2 == 0, me ^ masks[0], me ^ masks[1])


def expert_kernel(count, slots, gain_ref, wg_ref, wu_ref, wd_ref, tally_in, *refs):
    blocks, metas = refs[:count], refs[count : 2 * count]
    outs, tally_ref, normed = refs[2 * count : 3 * count], refs[3 * count], refs[3 * count + 1]
    rows = blocks[0].shape[0]
    me = lax.axis_index("tp")
    before = before_mask(rows)
    kinds = lax.broadcasted_iota(jnp.int32, (LANES, rows), 0)
    seen = jnp.zeros((LANES, rows), F32)
    for i, block in enumerate(blocks):
        first, second = metas[i][0:1, :], metas[i][1:2, :]
        seen = seen + jnp.where((first == kinds) | (second == kinds), 1.0, 0.0)
        pick = places(first, second, me, slots, before).astype(BF16)
        normed[i * slots : (i + 1) * slots, :] = layer_normed(dot(pick, block[...]), gain_ref[...])
    tally_ref[...] = tally_in[...] + dot(
        jnp.ones((8, rows), BF16), seen.astype(BF16), ((1,), (1,))
    )
    gate = dot(normed[...], wg_ref[...])
    up = dot(normed[...], wu_ref[...])
    hidden = (silu(gate) * up).astype(BF16)
    result = dot(hidden, wd_ref[...]).astype(BF16)
    for i, out in enumerate(outs):
        out[...] = result[i * slots : (i + 1) * slots]


def expert_call(gain, weights, tally, blocks, metas, slots):
    count = len(blocks)
    width, units = weights[0].shape
    return pl.pallas_call(
        functools.partial(expert_kernel, count, slots),
        out_shape=[jax.ShapeDtypeStruct((slots, width), BF16)] * count
        + [jax.ShapeDtypeStruct((8, LANES), F32)],
        in_specs=[VMEM] * (5 + 2 * count),
        out_specs=[VMEM] * (count + 1),
        scratch_shapes=[pltpu.VMEM((count * slots, width), BF16)],
        compiler_params=pltpu.CompilerParams(vmem_limit_bytes=24 * 2**20),
        cost_estimate=pl.CostEstimate(
            flops=6 * count * slots * width * units, bytes_accessed=6 * width * units, transcendentals=0
        ),
        name="expert_rows",
    )(gain, *weights, tally, *blocks, *metas)


def load_kernel(*refs):
    sources, targets, sems = refs[:3], refs[3:6], refs[6]
    copies = []
    for i, (source, target) in enumerate(zip(sources, targets)):
        part = target.shape[0] // 4
        for j in range(4):
            piece = pl.ds(j * part, part)
            copies.append(
                pltpu.make_async_copy(source.at[0, piece], target.at[piece], sems.at[i, j])
            )
    for copy in copies:
        copy.start()
    for copy in copies:
        copy.wait()


def load_call(*weights):
    return pl.pallas_call(
        load_kernel,
        out_shape=[jax.ShapeDtypeStruct(w.shape[1:], w.dtype) for w in weights],
        in_specs=[pl.BlockSpec(memory_space=pltpu.HBM)] * 3,
        out_specs=[VMEM] * 3,
        scratch_shapes=[pltpu.SemaphoreType.DMA((3, 4))],
        compiler_params=pltpu.CompilerParams(vmem_limit_bytes=16 * 2**20),
        name="load_weights",
    )(*[pltpu.with_memory_space_constraint(w, pltpu.HBM) for w in weights])


def shared_kernel(tokens_ref, gain_ref, wg_ref, wu_ref, wd_ref, out_ref):
    normed = layer_normed(tokens_ref[...].astype(F32), gain_ref[...])
    hidden = (silu(dot(normed, wg_ref[...])) * dot(normed, wu_ref[...])).astype(BF16)
    out_ref[...] = dot(hidden, wd_ref[...])


def combine_kernel(origins, routes_ref, gates_ref, base_ref, *refs):
    blocks, out_ref = refs[: len(origins)], refs[len(origins)]
    rows = base_ref.shape[0]
    first, second = routes_ref[0:1, :], routes_ref[1:2, :]
    before = before_mask(rows)
    lefts, rights = [], []
    for block, masks in zip(blocks, origins):
        expert = origin_id(masks)
        pick = places(first, second, expert, block.shape[0], before)
        left = jnp.where(first == expert, pick, 0.0)
        lefts.append(left.astype(BF16))
        rights.append((pick - left).astype(BF16))
    values = jnp.concatenate([block[...] for block in blocks], axis=0)
    gates = gates_ref[...].T
    total = base_ref[...]
    for k, picks in enumerate((lefts, rights)):
        chosen = dot(jnp.concatenate(picks, axis=0), values, ((0,), (0,)))
        total = total + gates[:, k : k + 1] * chosen
    out_ref[...] = total.astype(out_ref.dtype)


def combine_call(origins, routes, gates, base, blocks, kind):
    return pl.pallas_call(
        functools.partial(combine_kernel, origins),
        out_shape=jax.ShapeDtypeStruct(base.shape, kind),
        in_specs=[VMEM] * (3 + len(blocks)),
        out_specs=VMEM,
        compiler_params=pltpu.CompilerParams(vmem_limit_bytes=24 * 2**20),
        name="combine_rows",
    )(routes, gates, base, *blocks)


def per_device(
    tokens,
    norm_gain,
    routes,
    gates,
    expert_gate,
    expert_up,
    expert_down,
    shared_gate,
    shared_up,
    shared_down,
):
    rows, width = tokens.shape
    top = routes.shape[1]
    groups, planes = lax.axis_size("tp"), lax.axis_size("ep")
    slots = 2 * rows * top // groups
    ids = np.arange(groups)
    partner = ids ^ 1
    gain = norm_gain.reshape(1, width)
    routes, gates = routes.T, gates.T

    def send(value, perm):
        return lax.ppermute(value, "tp", [(int(i), int(perm[i])) for i in ids])

    def masks_of(perm):
        return int(perm[0]), int(perm[1] ^ 1)

    masks = [1 << b for b in range(1, groups.bit_length() - 1)]
    hops = [
        np.where(ids % 2 == 0, ids ^ masks[i], ids ^ masks[-1 - i]) for i in range(len(masks))
    ]
    known, metas = [(tokens, ids)], [(routes, ids)]
    for hop in hops:
        for block, origin in list(known):
            known.append((send(block, hop), origin[hop]))
            metas.append((send(routes, origin[hop]), origin[hop]))
    weights = load_call(expert_gate, expert_up, expert_down)

    tally = jnp.zeros((8, LANES), F32)
    returned = []

    def run(block, meta, origin, tally):
        across = send(block, partner)
        meta_across = send(meta, partner)
        *results, tally = expert_call(
            gain, weights, tally, [block, across], [meta, meta_across], slots
        )
        back = []
        for result, source in zip(results, (origin, origin[partner])):
            if np.array_equal(source, ids):
                back.append((result, ids))
            else:
                back.append((send(result, source), np.argsort(source)))
        returned.append(back)
        return tally

    for number in (*range(1, len(known)), 0):
        tally = run(known[number][0], *metas[number], tally)

    base = pl.pallas_call(
        shared_kernel,
        out_shape=jax.ShapeDtypeStruct((rows, width), F32),
        in_specs=[VMEM] * 5,
        out_specs=VMEM,
        compiler_params=pltpu.CompilerParams(vmem_limit_bytes=24 * 2**20),
        name="shared_rows",
    )(tokens, gain, shared_gate, shared_up, shared_down)

    late = returned.pop(-2) if len(returned) > 1 else []
    early = [item for back in returned for item in back]
    for blocks, kind in ((early, F32), (late, BF16)):
        origins = [masks_of(origin) for _, origin in blocks]
        base = combine_call(origins, routes, gates, base, [b for b, _ in blocks], kind)

    total = tally[0:1]
    if planes & (planes - 1):
        total = lax.psum(total, "ep")
    else:
        for bit in range(planes.bit_length() - 1):
            other = lax.ppermute(total, "ep", [(i, i ^ (1 << bit)) for i in range(planes)])
            total = total + other
    load = total[0, :groups] * (groups / (rows * top * planes * groups))
    return base, load


def solution(mesh):
    placed = (
        P(("ep", "tp"), None),
        P(),
        P(("ep", "tp"), None),
        P(("ep", "tp"), None),
        P("tp", None, None),
        P("tp", None, None),
        P("tp", None, None),
        P(),
        P(),
        P(),
    )

    return jax.shard_map(
        per_device,
        mesh=mesh,
        in_specs=placed,
        out_specs=(P(("ep", "tp"), None), P()),
        check_vma=False,
    )
```

```python
import functools

import jax
import jax.numpy as jnp
import numpy as np
from jax import lax
from jax.experimental import pallas as pl
from jax.experimental.pallas import tpu as pltpu
from jax.sharding import PartitionSpec as P

LANES = 128
VMEM = pl.BlockSpec(memory_space=pltpu.VMEM)
F32 = jnp.float32
BF16 = jnp.bfloat16


def dot(a, b, contract=((1,), (0,))):
    return lax.dot_general(a, b, (contract, ((), ())), preferred_element_type=F32)


def layer_normed(values, gain):
    center = jnp.mean(values, axis=-1, keepdims=True)
    moved = values - center
    spread = jnp.mean(moved * moved, axis=-1, keepdims=True)
    return (moved * lax.rsqrt(spread + 1e-05) * gain).astype(BF16)


def silu(v):
    return v / (1.0 + jnp.exp(-v))


def before_mask(rows):
    row = lax.broadcasted_iota(jnp.int32, (rows, rows), 0)
    col = lax.broadcasted_iota(jnp.int32, (rows, rows), 1)
    return jnp.where(row < col, 1.0, 0.0).astype(BF16)


def places(first, second, expert, slots, before):
    rows = first.shape[1]
    named = jnp.where((first == expert) | (second == expert), 1.0, 0.0)
    rank = dot(jnp.broadcast_to(named, (8, rows)).astype(BF16), before)[0:1]
    slot = lax.broadcasted_iota(jnp.int32, (slots, rows), 0).astype(F32)
    return jnp.where((rank == slot) & (named > 0.0), 1.0, 0.0)


def origin_id(masks):
    me = lax.axis_index("tp")
    return jnp.where(me % 2 == 0, me ^ masks[0], me ^ masks[1])


def expert_kernel(count, slots, halves, gain_ref, wg_ref, wu_ref, wd_ref, *refs):
    blocks, metas = refs[:count], refs[count : 2 * count]
    outs, normed = refs[2 * count : 3 * count], refs[3 * count]
    rows = blocks[0].shape[0]
    me = lax.axis_index("tp")
    before = before_mask(rows)
    for i, block in enumerate(blocks):
        at = 2 * halves[i]
        pick = places(metas[i][at : at + 1, :], metas[i][at + 1 : at + 2, :], me, slots, before)
        normed[i * slots : (i + 1) * slots, :] = layer_normed(
            dot(pick.astype(BF16), block[...]), gain_ref[...]
        )
    gate = dot(normed[...], wg_ref[...])
    up = dot(normed[...], wu_ref[...])
    hidden = (silu(gate) * up).astype(BF16)
    result = dot(hidden, wd_ref[...]).astype(BF16)
    for i, out in enumerate(outs):
        out[...] = result[i * slots : (i + 1) * slots]


def expert_call(gain, weights, blocks, metas, halves, slots):
    count = len(blocks)
    width, units = weights[0].shape
    return pl.pallas_call(
        functools.partial(expert_kernel, count, slots, halves),
        out_shape=[jax.ShapeDtypeStruct((slots, width), BF16)] * count,
        in_specs=[VMEM] * (4 + 2 * count),
        out_specs=[VMEM] * count,
        scratch_shapes=[pltpu.VMEM((count * slots, width), BF16)],
        compiler_params=pltpu.CompilerParams(vmem_limit_bytes=24 * 2**20),
        cost_estimate=pl.CostEstimate(
            flops=6 * count * slots * width * units, bytes_accessed=6 * width * units, transcendentals=0
        ),
        name="expert_rows",
    )(gain, *weights, *blocks, *metas)


def pair_kernel(mine_ref, other_ref, out_ref):
    top = mine_ref.shape[0]
    out_ref[0:top, :] = mine_ref[...]
    out_ref[top:, :] = other_ref[...]


def pair_call(mine, other):
    return pl.pallas_call(
        pair_kernel,
        out_shape=jax.ShapeDtypeStruct((2 * mine.shape[0], mine.shape[1]), mine.dtype),
        in_specs=[VMEM] * 2,
        out_specs=VMEM,
        compiler_params=pltpu.CompilerParams(vmem_limit_bytes=4 * 2**20),
        name="pair_routes",
    )(mine, other)


def tally_kernel(*refs):
    metas, out_ref = refs[:-1], refs[-1]
    rows = metas[0].shape[1]
    kinds = lax.broadcasted_iota(jnp.int32, (LANES, rows), 0)
    seen = jnp.zeros((LANES, rows), F32)
    for meta in metas:
        for i in range(meta.shape[0]):
            seen = seen + jnp.where(meta[i : i + 1, :] == kinds, 1.0, 0.0)
    out_ref[...] = dot(jnp.ones((8, rows), BF16), seen.astype(BF16), ((1,), (1,)))


def tally_call(metas):
    return pl.pallas_call(
        tally_kernel,
        out_shape=jax.ShapeDtypeStruct((8, LANES), F32),
        in_specs=[VMEM] * len(metas),
        out_specs=VMEM,
        compiler_params=pltpu.CompilerParams(vmem_limit_bytes=4 * 2**20),
        name="tally_routes",
    )(*metas)


def load_kernel(count, *refs):
    sources, targets, sems = refs[:count], refs[count : 2 * count], refs[2 * count]
    copies = []
    for i, (source, target) in enumerate(zip(sources, targets)):
        part = target.shape[0] // 4
        for j in range(4):
            piece = pl.ds(j * part, part)
            copies.append(
                pltpu.make_async_copy(source.at[0, piece], target.at[piece], sems.at[i, j])
            )
    for copy in copies:
        copy.start()
    for copy in copies:
        copy.wait()


def load_call(*weights):
    count = len(weights)
    return pl.pallas_call(
        functools.partial(load_kernel, count),
        out_shape=[jax.ShapeDtypeStruct(w.shape[1:], w.dtype) for w in weights],
        in_specs=[pl.BlockSpec(memory_space=pltpu.HBM)] * count,
        out_specs=[VMEM] * count,
        scratch_shapes=[pltpu.SemaphoreType.DMA((count, 4))],
        compiler_params=pltpu.CompilerParams(vmem_limit_bytes=16 * 2**20),
        name="load_weights",
    )(*[pltpu.with_memory_space_constraint(w, pltpu.HBM) for w in weights])


def shared_kernel(tokens_ref, gain_ref, wg_ref, wu_ref, wd_ref, out_ref):
    normed = layer_normed(tokens_ref[...].astype(F32), gain_ref[...])
    hidden = (silu(dot(normed, wg_ref[...])) * dot(normed, wu_ref[...])).astype(BF16)
    out_ref[...] = dot(hidden, wd_ref[...])


def picks_of(routes_ref, origins, slots, before):
    first, second = routes_ref[0:1, :], routes_ref[1:2, :]
    lefts, rights = [], []
    for masks in origins:
        expert = origin_id(masks)
        pick = places(first, second, expert, slots, before)
        left = jnp.where(first == expert, pick, 0.0)
        lefts.append(left)
        rights.append(pick - left)
    stack = [jnp.concatenate(part, axis=0).T for part in (lefts, rights)]
    return jnp.concatenate(stack, axis=0).astype(BF16)


def combine_kernel(early, late, routes_ref, gates_ref, base_ref, *refs):
    blocks, (out_ref, picks_ref, gates_out) = refs[:-3], refs[-3:]
    rows, slots = base_ref.shape[0], blocks[0].shape[0]
    before = before_mask(rows)
    gates = gates_ref[...].T
    gates_out[...] = gates
    picks_ref[...] = picks_of(routes_ref, late, slots, before)
    values = jnp.concatenate([block[...] for block in blocks], axis=0)
    chosen = dot(picks_of(routes_ref, early, slots, before), values)
    out_ref[...] = (
        base_ref[...] + gates[:, 0:1] * chosen[:rows] + gates[:, 1:2] * chosen[rows:]
    )


def finish_kernel(pieces, picks_ref, gates_ref, base_ref, *refs):
    blocks, (out_ref, mixed, sems) = refs[:-3], refs[-3:]
    rows, width = base_ref.shape
    part = width // pieces
    copies = []
    for j in range(pieces):
        cols = slice(j * part, (j + 1) * part)
        values = jnp.concatenate([block[:, cols] for block in blocks], axis=0)
        chosen = dot(picks_ref[...], values)
        total = base_ref[:, cols] + gates_ref[:, 0:1] * chosen[:rows]
        mixed[:, cols] = (total + gates_ref[:, 1:2] * chosen[rows:]).astype(mixed.dtype)
        copies.append(pltpu.make_async_copy(mixed.at[:, cols], out_ref.at[:, cols], sems.at[j]))
        copies[-1].start()
    for copy in copies:
        copy.wait()


def combine_call(early, late, routes, gates, base, blocks):
    rows, slots = base.shape[0], blocks[0].shape[0]
    return pl.pallas_call(
        functools.partial(combine_kernel, early, late),
        out_shape=[
            jax.ShapeDtypeStruct(base.shape, F32),
            jax.ShapeDtypeStruct((2 * rows, slots * len(late)), BF16),
            jax.ShapeDtypeStruct((rows, gates.shape[0]), F32),
        ],
        in_specs=[VMEM] * (3 + len(blocks)),
        out_specs=[VMEM] * 3,
        compiler_params=pltpu.CompilerParams(vmem_limit_bytes=24 * 2**20),
        name="combine_rows",
    )(routes, gates, base, *blocks)


def finish_call(picks, gates, base, blocks, pieces=4):
    return pl.pallas_call(
        functools.partial(finish_kernel, pieces),
        out_shape=jax.ShapeDtypeStruct(base.shape, BF16),
        in_specs=[VMEM] * (3 + len(blocks)),
        out_specs=pl.BlockSpec(memory_space=pltpu.HBM),
        scratch_shapes=[pltpu.VMEM(base.shape, BF16), pltpu.SemaphoreType.DMA((pieces,))],
        compiler_params=pltpu.CompilerParams(vmem_limit_bytes=24 * 2**20),
        name="finish_rows",
    )(picks, gates, base, *blocks)


def per_device(
    tokens,
    norm_gain,
    routes,
    gates,
    expert_gate,
    expert_up,
    expert_down,
    shared_gate,
    shared_up,
    shared_down,
):
    rows, width = tokens.shape
    top = routes.shape[1]
    groups, planes = lax.axis_size("tp"), lax.axis_size("ep")
    slots = 2 * rows * top // groups
    ids = np.arange(groups)
    partner = ids ^ 1
    gain = norm_gain.reshape(1, width)
    routes, gates = routes.T, gates.T

    def send(value, perm):
        return lax.ppermute(value, "tp", [(int(i), int(perm[i])) for i in ids])

    def masks_of(perm):
        return int(perm[0]), int(perm[1] ^ 1)

    masks = [1 << b for b in range(1, groups.bit_length() - 1)]
    hops = [
        np.where(ids % 2 == 0, ids ^ masks[i], ids ^ masks[-1 - i]) for i in range(len(masks))
    ]
    both = pair_call(routes, send(routes, partner))
    known, metas = [(tokens, ids)], [both]
    for hop in hops:
        for block, origin in list(known):
            known.append((send(block, hop), origin[hop]))
            metas.append(send(both, origin[hop]))
    weights = load_call(expert_gate, expert_up) + load_call(expert_down)
    total = tally_call(metas)[0:1]

    def meta_of(source):
        for meta, (_, origin) in zip(metas, known):
            if np.array_equal(origin, source):
                return meta, 0
            if np.array_equal(origin ^ 1, source):
                return meta, 1

    returned = []
    for number in (*range(1, len(known)), 0):
        block, origin = known[number]
        across = send(block, partner)
        sources = (origin, origin[partner])
        found = [meta_of(source) for source in sources]
        results = expert_call(
            gain, weights, [block, across], [m for m, _ in found], [h for _, h in found], slots
        )
        back = []
        for result, source in zip(results, sources):
            if np.array_equal(source, ids):
                back.append((result, ids))
            else:
                back.append((send(result, source), np.argsort(source)))
        returned.append(back)

    base = pl.pallas_call(
        shared_kernel,
        out_shape=jax.ShapeDtypeStruct((rows, width), F32),
        in_specs=[VMEM] * 5,
        out_specs=VMEM,
        compiler_params=pltpu.CompilerParams(vmem_limit_bytes=24 * 2**20),
        name="shared_rows",
    )(tokens, gain, shared_gate, shared_up, shared_down)

    late = returned.pop(-2)
    if len(returned) > 2:
        late = returned.pop(-2) + late
    early = [item for back in returned for item in back]
    base, picks, columns = combine_call(
        [masks_of(origin) for _, origin in early],
        [masks_of(origin) for _, origin in late],
        routes,
        gates,
        base,
        [block for block, _ in early],
    )
    mixed = finish_call(picks, columns, base, [block for block, _ in late])

    if planes & (planes - 1):
        total = lax.psum(total, "ep")
    else:
        for bit in range(planes.bit_length() - 1):
            other = lax.ppermute(total, "ep", [(i, i ^ (1 << bit)) for i in range(planes)])
            total = total + other
    load = total[0, :groups] * (groups / (rows * top * planes * groups))
    return mixed, load


def solution(mesh):
    placed = (
        P(("ep", "tp"), None),
        P(),
        P(("ep", "tp"), None),
        P(("ep", "tp"), None),
        P("tp", None, None),
        P("tp", None, None),
        P("tp", None, None),
        P(),
        P(),
        P(),
    )

    return jax.shard_map(
        per_device,
        mesh=mesh,
        in_specs=placed,
        out_specs=(P(("ep", "tp"), None), P()),
        check_vma=False,
    )
```

```python
import functools

import jax
import jax.numpy as jnp
import numpy as np
from jax import lax
from jax.experimental import pallas as pl
from jax.experimental.pallas import tpu as pltpu
from jax.sharding import PartitionSpec as P

LANES = 128
VMEM = pl.BlockSpec(memory_space=pltpu.VMEM)
F32 = jnp.float32
BF16 = jnp.bfloat16


def dot(a, b, contract=((1,), (0,))):
    return lax.dot_general(a, b, (contract, ((), ())), preferred_element_type=F32)


def layer_normed(values, gain):
    center = jnp.mean(values, axis=-1, keepdims=True)
    moved = values - center
    spread = jnp.mean(moved * moved, axis=-1, keepdims=True)
    return (moved * lax.rsqrt(spread + 1e-05) * gain).astype(BF16)


def silu(v):
    return v / (1.0 + jnp.exp(-v))


def before_mask(rows):
    row = lax.broadcasted_iota(jnp.int32, (rows, rows), 0)
    col = lax.broadcasted_iota(jnp.int32, (rows, rows), 1)
    return jnp.where(row < col, 1.0, 0.0).astype(BF16)


def places(first, second, expert, slots, before):
    rows = first.shape[1]
    named = jnp.where((first == expert) | (second == expert), 1.0, 0.0)
    rank = dot(jnp.broadcast_to(named, (8, rows)).astype(BF16), before)[0:1]
    slot = lax.broadcasted_iota(jnp.int32, (slots, rows), 0).astype(F32)
    return jnp.where((rank == slot) & (named > 0.0), 1.0, 0.0)


def origin_id(masks):
    me = lax.axis_index("tp")
    return jnp.where(me % 2 == 0, me ^ masks[0], me ^ masks[1])


def expert_kernel(count, slots, halves, gain_ref, wg_ref, wu_ref, wd_ref, *refs):
    blocks, metas = refs[:count], refs[count : 2 * count]
    outs, normed = refs[2 * count : 3 * count], refs[3 * count]
    rows = blocks[0].shape[0]
    me = lax.axis_index("tp")
    before = before_mask(rows)
    for i, block in enumerate(blocks):
        at = 2 * halves[i]
        pick = places(metas[i][at : at + 1, :], metas[i][at + 1 : at + 2, :], me, slots, before)
        normed[i * slots : (i + 1) * slots, :] = layer_normed(
            dot(pick.astype(BF16), block[...]), gain_ref[...]
        )
    gate = dot(normed[...], wg_ref[...])
    up = dot(normed[...], wu_ref[...])
    hidden = (silu(gate) * up).astype(BF16)
    result = dot(hidden, wd_ref[...]).astype(BF16)
    for i, out in enumerate(outs):
        out[...] = result[i * slots : (i + 1) * slots]


def expert_call(gain, weights, blocks, metas, halves, slots):
    count = len(blocks)
    width, units = weights[0].shape
    return pl.pallas_call(
        functools.partial(expert_kernel, count, slots, halves),
        out_shape=[jax.ShapeDtypeStruct((slots, width), BF16)] * count,
        in_specs=[VMEM] * (4 + 2 * count),
        out_specs=[VMEM] * count,
        scratch_shapes=[pltpu.VMEM((count * slots, width), BF16)],
        compiler_params=pltpu.CompilerParams(vmem_limit_bytes=24 * 2**20),
        cost_estimate=pl.CostEstimate(
            flops=6 * count * slots * width * units, bytes_accessed=6 * width * units, transcendentals=0
        ),
        name="expert_rows",
    )(gain, *weights, *blocks, *metas)


def pair_kernel(mine_ref, other_ref, out_ref):
    top = mine_ref.shape[0]
    out_ref[0:top, :] = mine_ref[...]
    out_ref[top:, :] = other_ref[...]


def pair_call(mine, other):
    return pl.pallas_call(
        pair_kernel,
        out_shape=jax.ShapeDtypeStruct((2 * mine.shape[0], mine.shape[1]), mine.dtype),
        in_specs=[VMEM] * 2,
        out_specs=VMEM,
        compiler_params=pltpu.CompilerParams(vmem_limit_bytes=4 * 2**20),
        name="pair_routes",
    )(mine, other)


def tally_kernel(*refs):
    metas, out_ref = refs[:-1], refs[-1]
    rows = metas[0].shape[1]
    kinds = lax.broadcasted_iota(jnp.int32, (LANES, rows), 0)
    seen = jnp.zeros((LANES, rows), F32)
    for meta in metas:
        for i in range(meta.shape[0]):
            seen = seen + jnp.where(meta[i : i + 1, :] == kinds, 1.0, 0.0)
    out_ref[...] = dot(jnp.ones((8, rows), BF16), seen.astype(BF16), ((1,), (1,)))


def tally_call(metas):
    return pl.pallas_call(
        tally_kernel,
        out_shape=jax.ShapeDtypeStruct((8, LANES), F32),
        in_specs=[VMEM] * len(metas),
        out_specs=VMEM,
        compiler_params=pltpu.CompilerParams(vmem_limit_bytes=4 * 2**20),
        name="tally_routes",
    )(*metas)


def load_kernel(count, *refs):
    sources, targets, sems = refs[:count], refs[count : 2 * count], refs[2 * count]
    copies = []
    for i, (source, target) in enumerate(zip(sources, targets)):
        part = target.shape[0] // 8
        for j in range(8):
            piece = pl.ds(j * part, part)
            copies.append(
                pltpu.make_async_copy(source.at[0, piece], target.at[piece], sems.at[i, j])
            )
    for copy in copies:
        copy.start()
    for copy in copies:
        copy.wait()


def load_call(*weights):
    count = len(weights)
    return pl.pallas_call(
        functools.partial(load_kernel, count),
        out_shape=[jax.ShapeDtypeStruct(w.shape[1:], w.dtype) for w in weights],
        in_specs=[pl.BlockSpec(memory_space=pltpu.HBM)] * count,
        out_specs=[VMEM] * count,
        scratch_shapes=[pltpu.SemaphoreType.DMA((count, 8))],
        compiler_params=pltpu.CompilerParams(vmem_limit_bytes=16 * 2**20),
        name="load_weights",
    )(*[pltpu.with_memory_space_constraint(w, pltpu.HBM) for w in weights])


def shared_kernel(tokens_ref, gain_ref, wg_ref, wu_ref, wd_ref, out_ref):
    normed = layer_normed(tokens_ref[...].astype(F32), gain_ref[...])
    hidden = (silu(dot(normed, wg_ref[...])) * dot(normed, wu_ref[...])).astype(BF16)
    out_ref[...] = dot(hidden, wd_ref[...])


def picks_of(routes_ref, origins, slots, before):
    first, second = routes_ref[0:1, :], routes_ref[1:2, :]
    lefts, rights = [], []
    for masks in origins:
        expert = origin_id(masks)
        pick = places(first, second, expert, slots, before)
        left = jnp.where(first == expert, pick, 0.0)
        lefts.append(left)
        rights.append(pick - left)
    stack = [jnp.concatenate(part, axis=0).T for part in (lefts, rights)]
    return jnp.concatenate(stack, axis=0).astype(BF16)


def combine_kernel(early, late, routes_ref, gates_ref, base_ref, *refs):
    blocks, (out_ref, picks_ref, gates_out, last_ref, gate_ref) = refs[:-5], refs[-5:]
    rows, slots = base_ref.shape[0], blocks[0].shape[0]
    before = before_mask(rows)
    gates = gates_ref[...].T
    gates_out[...] = gates
    picks_ref[...] = picks_of(routes_ref, late[:-1], slots, before)
    first, second = routes_ref[0:1, :], routes_ref[1:2, :]
    expert = origin_id(late[-1])
    last_ref[...] = places(first, second, expert, slots, before).T.astype(BF16)
    scale = jnp.where(first == expert, gates_ref[0:1, :], gates_ref[1:2, :])
    gate_ref[...] = jnp.broadcast_to(scale, (8, rows)).T[:, 0:1]
    values = jnp.concatenate([block[...] for block in blocks], axis=0)
    chosen = dot(picks_of(routes_ref, early, slots, before), values)
    out_ref[...] = (
        base_ref[...] + gates[:, 0:1] * chosen[:rows] + gates[:, 1:2] * chosen[rows:]
    )


def combine_call(early, late, routes, gates, base, blocks):
    rows, slots = base.shape[0], blocks[0].shape[0]
    return pl.pallas_call(
        functools.partial(combine_kernel, early, late),
        out_shape=[
            jax.ShapeDtypeStruct(base.shape, F32),
            jax.ShapeDtypeStruct((2 * rows, slots * (len(late) - 1)), BF16),
            jax.ShapeDtypeStruct((rows, gates.shape[0]), F32),
            jax.ShapeDtypeStruct((rows, slots), BF16),
            jax.ShapeDtypeStruct((rows, 1), F32),
        ],
        in_specs=[VMEM] * (3 + len(blocks)),
        out_specs=[VMEM] * 5,
        compiler_params=pltpu.CompilerParams(vmem_limit_bytes=24 * 2**20),
        name="combine_rows",
    )(routes, gates, base, *blocks)


def middle_kernel(picks_ref, gates_ref, base_ref, *refs):
    blocks, out_ref = refs[:-1], refs[-1]
    rows = base_ref.shape[0]
    values = jnp.concatenate([block[...] for block in blocks], axis=0)
    chosen = dot(picks_ref[...], values)
    total = base_ref[...] + gates_ref[:, 0:1] * chosen[:rows]
    out_ref[...] = total + gates_ref[:, 1:2] * chosen[rows:]


def middle_call(picks, gates, base, blocks):
    return pl.pallas_call(
        middle_kernel,
        out_shape=jax.ShapeDtypeStruct(base.shape, F32),
        in_specs=[VMEM] * (3 + len(blocks)),
        out_specs=VMEM,
        compiler_params=pltpu.CompilerParams(vmem_limit_bytes=24 * 2**20),
        name="middle_rows",
    )(picks, gates, base, *blocks)


def finish_kernel(pieces, pick_ref, gate_ref, base_ref, block_ref, out_ref, mixed, sems):
    part = base_ref.shape[1] // pieces
    gate = gate_ref[...]
    copies = []
    for j in range(pieces):
        cols = slice(j * part, (j + 1) * part)
        total = base_ref[:, cols] + gate * dot(pick_ref[...], block_ref[:, cols])
        mixed[:, cols] = total.astype(mixed.dtype)
        copies.append(pltpu.make_async_copy(mixed.at[:, cols], out_ref.at[:, cols], sems.at[j]))
        copies[-1].start()
    for copy in copies:
        copy.wait()


def finish_call(pick, gate, base, block, pieces=4):
    return pl.pallas_call(
        functools.partial(finish_kernel, pieces),
        out_shape=jax.ShapeDtypeStruct(base.shape, BF16),
        in_specs=[VMEM] * 4,
        out_specs=pl.BlockSpec(memory_space=pltpu.HBM),
        scratch_shapes=[pltpu.VMEM(base.shape, BF16), pltpu.SemaphoreType.DMA((pieces,))],
        compiler_params=pltpu.CompilerParams(vmem_limit_bytes=24 * 2**20),
        name="finish_rows",
    )(pick, gate, base, block)


def per_device(
    tokens,
    norm_gain,
    routes,
    gates,
    expert_gate,
    expert_up,
    expert_down,
    shared_gate,
    shared_up,
    shared_down,
):
    rows, width = tokens.shape
    top = routes.shape[1]
    groups, planes = lax.axis_size("tp"), lax.axis_size("ep")
    slots = 2 * rows * top // groups
    ids = np.arange(groups)
    partner = ids ^ 1
    gain = norm_gain.reshape(1, width)
    routes, gates = routes.T, gates.T

    def send(value, perm):
        return lax.ppermute(value, "tp", [(int(i), int(perm[i])) for i in ids])

    def masks_of(perm):
        return int(perm[0]), int(perm[1] ^ 1)

    masks = [1 << b for b in range(1, groups.bit_length() - 1)]
    hops = [
        np.where(ids % 2 == 1, ids ^ masks[i], ids ^ masks[-1 - i]) for i in range(len(masks))
    ]
    both = pair_call(routes, send(routes, partner))
    known, metas = [(tokens, ids)], [both]
    for hop in hops:
        for block, origin in list(known):
            known.append((send(block, hop), origin[hop]))
            metas.append(send(both, origin[hop]))
    weights = load_call(expert_gate, expert_up) + load_call(expert_down)
    total = tally_call(metas)[0:1]

    def meta_of(source):
        for meta, (_, origin) in zip(metas, known):
            if np.array_equal(origin, source):
                return meta, 0
            if np.array_equal(origin ^ 1, source):
                return meta, 1

    returned = []
    for number in (*range(1, len(known)), 0):
        block, origin = known[number]
        across = send(block, partner)
        sources = (origin, origin[partner])
        found = [meta_of(source) for source in sources]
        results = expert_call(
            gain, weights, [block, across], [m for m, _ in found], [h for _, h in found], slots
        )
        back = []
        for result, source in zip(results, sources):
            if np.array_equal(source, ids):
                back.append((result, ids))
            else:
                back.append((send(result, source), np.argsort(source)))
        returned.append(back)

    base = pl.pallas_call(
        shared_kernel,
        out_shape=jax.ShapeDtypeStruct((rows, width), F32),
        in_specs=[VMEM] * 5,
        out_specs=VMEM,
        compiler_params=pltpu.CompilerParams(vmem_limit_bytes=24 * 2**20),
        name="shared_rows",
    )(tokens, gain, shared_gate, shared_up, shared_down)

    late = returned.pop(-2)
    if len(returned) > 2:
        late = returned.pop(-2) + late
    early = [item for back in returned for item in back]
    base, picks, columns, pick, gate = combine_call(
        [masks_of(origin) for _, origin in early],
        [masks_of(origin) for _, origin in late],
        routes,
        gates,
        base,
        [block for block, _ in early],
    )
    base = middle_call(picks, columns, base, [block for block, _ in late[:-1]])
    mixed = finish_call(pick, gate, base, late[-1][0])

    if planes & (planes - 1):
        total = lax.psum(total, "ep")
    else:
        for bit in range(planes.bit_length() - 1):
            other = lax.ppermute(total, "ep", [(i, i ^ (1 << bit)) for i in range(planes)])
            total = total + other
    load = total[0, :groups] * (groups / (rows * top * planes * groups))
    return mixed, load


def solution(mesh):
    placed = (
        P(("ep", "tp"), None),
        P(),
        P(("ep", "tp"), None),
        P(("ep", "tp"), None),
        P("tp", None, None),
        P("tp", None, None),
        P("tp", None, None),
        P(),
        P(),
        P(),
    )

    return jax.shard_map(
        per_device,
        mesh=mesh,
        in_specs=placed,
        out_specs=(P(("ep", "tp"), None), P()),
        check_vma=False,
    )
```
